32 devices in a mesh: grp: 2 (over y), sp: 8 (over z, core), tp: 2 (over x).
Axes of the slice: x: 2, y: 2, z: 4, core: 2. Of those that a mesh axis runs over, the one named last changes fastest.
Arguments:
- tokens: bfloat16 [12288, 2048], P(('grp', 'sp'), 'tp'), parts along dimension 0, may hold values from -4000 to 4000
- gain: float32 [2048], replicated, may hold values from 0.1 to 1.9
- w_query: bfloat16 [2048, 1024], P('sp', 'tp'), may hold values from -1 to 1
- w_key: bfloat16 [2048, 256], P('sp', 'tp'), may hold values from -1 to 1
- w_value: bfloat16 [2048, 256], P('sp', 'tp'), may hold values from -0.125 to 0.125
- w_input: bfloat16 [2048, 1024], P('sp', 'tp'), may hold values from -0.125 to 0.125
- w_bgate: bfloat16 [2048, 1024], P('sp', 'tp'), may hold values from -0.125 to 0.125
- w_cgate: bfloat16 [2048, 1024], P('sp', 'tp'), may hold values from -0.125 to 0.125
- w_attn_out: bfloat16 [1024, 2048], P('sp', 'tp'), may hold values from -2 to 2
- w_conv_out: bfloat16 [1024, 2048], P('sp', 'tp'), may hold values from -0.1875 to 0.1875
- sink_logit: float32 [16], P('tp'), may hold values from 0 to 5
- taps: float32 [3, 1024], P(None, 'tp'), may hold values from -3.5 to 3.5
- conv_bias: float32 [1024], P('tp'), may hold values from -4 to 4
- documents: int32 [12288], P(('grp', 'sp')), parts along dimension 0, may hold values from 0 to 3, never falling along the last dimension, each value on 1 to 3072 neighbouring positions
Outputs:
- mixed: bfloat16 [12288, 2048], P(('grp', 'sp'), 'tp'), parts along dimension 0
The draws below stay inside these ranges and needn't reach their ends.
There are 2 independent parts, one for each index of `grp`. The reference program is written for one: setup_inputs(seed, part) draws one part's arguments, and reference() takes and returns one part's arrays. A program takes and returns all parts, laid end to end along the dimension named above; an argument that names none is the same for every part. Nothing has to cross between parts.
All inputs are finite; a program needn't handle non-finite values.
Results may differ from the reference program's by a relative error of at most 0.013.
The reference program's roundings to bfloat16 on the way (of `scaled`, `weight`, `attended`, `carried` and `convolved`) count: a program that leaves them out, or rounds other values in their place, can miss the bound.
Values may be sent and summed in bfloat16 or wider, within the bound.
A program may use at most 64 MiB of HBM per device.

```python
import math
import jax
import jax.numpy as jnp
import numpy as np
from jax import lax

D = 2048
Q_HEADS = 16
KV_HEADS = 4
HEAD_DIM = 64
CW = 1024
WINDOW = 128
TOK_DEV = 768
QW = 1024
KVW = 256
TOKENS = 6144
DOCS = 4


def draw_tokens(key, part):
    f32 = jnp.float32
    base = jnp.clip(jax.random.normal(jax.random.fold_in(key, 11), (TOKENS, D), f32), -6.0, 6.0)
    columns = jnp.exp(jax.random.uniform(jax.random.fold_in(key, 12), (D,), f32, 0.0, jnp.log(10.0)))
    order = jax.random.permutation(jax.random.fold_in(key, 13), 4).astype(f32)
    blocks = jnp.power(3.0, order / 3.0)
    block_of = (jnp.arange(D) // (D // 4)).astype(jnp.int32)
    columns = columns * blocks[block_of]
    rows = jnp.exp(jax.random.uniform(jax.random.fold_in(key, 14), (TOKENS, 1), f32, 0.0, jnp.log(10.0)))
    values = base * columns[None, :] * rows
    return values.astype(jnp.bfloat16)


def query_parts(key):
    f32 = jnp.float32
    base = jnp.clip(jax.random.normal(jax.random.fold_in(key, 101), (D, Q_HEADS * HEAD_DIM), f32), -6.0, 6.0) * D ** (-0.5)
    return base


def draw_w_query(key, part):
    base = query_parts(key)
    values = base
    return jnp.clip(values, -1.0, 1.0).astype(jnp.bfloat16)


def draw_w_key(key, part):
    f32 = jnp.float32
    values = jnp.clip(jax.random.normal(jax.random.fold_in(key, 202), (D, KV_HEADS * HEAD_DIM), f32), -6.0, 6.0) * D ** (-0.5)
    return jnp.clip(values, -1.0, 1.0).astype(jnp.bfloat16)


def steps_of(stream_key, dims, cuts, least, top_value):
    def one(axis_at, blocks):
        steps = jax.random.uniform(jax.random.fold_in(jax.random.fold_in(stream_key, 6), axis_at), (blocks,), jnp.float32, least / len(cuts), top_value / len(cuts))
        return jnp.repeat(jnp.exp(steps), dims[axis_at] // blocks).reshape((-1,) + (1,) * (len(dims) - axis_at - 1))

    level = one(*cuts[0])
    for cut in cuts[1:]:
        level = level * one(*cut)
    return level


def split_up(number_of, total, reach, slope):
    weights = [(1 << 20) // math.isqrt(grade ** slope) + 1 for grade in range(2, number_of + 1)]
    rest, given = total - reach - (number_of - 1), [1] * (number_of - 1)
    while rest > 0:
        free = [i for i in range(number_of - 1) if given[i] < reach]
        whole, remaining = sum([weights[i] for i in free]), rest
        for i in free:
            addition = min(reach - given[i], max(1, remaining * weights[i] // whole), rest)
            given[i] = given[i] + addition
            rest = rest - addition
    return np.array([reach] + given)


def uneven(own_key, amount, total, limit, lean):
    if amount == 2:
        one = jax.random.randint(own_key, (), max(1, total - limit), min(limit, total - 1) + 1)
        return jnp.stack([one, total - one])
    sizes = jnp.asarray(split_up(amount, total, limit, lean), jnp.int32)
    twos = (amount - 1) // 2
    donor, receiver = sizes[1:1 + 2 * twos:2], sizes[2:2 + 2 * twos:2]
    slack = jnp.minimum(donor - 1, limit - receiver)
    shifted = jax.random.randint(jax.random.fold_in(own_key, 1), (twos,), 0, 1 << 20) % (slack + 1)
    sizes = sizes.at[1:1 + 2 * twos:2].set(donor - shifted).at[2:2 + 2 * twos:2].set(receiver + shifted)
    return sizes[jax.random.permutation(jax.random.fold_in(own_key, 2), amount)]


def centred(rng, dims, spread, most, cuts=(), kind=jnp.bfloat16):
    result = spread * jax.random.normal(rng, dims, jnp.float32)
    if cuts:
        result = result * steps_of(rng, dims, cuts, -0.22, 0.18)
    return jnp.clip(result, -most, most).astype(kind)


def setup_inputs(seed: int = 0, part: int = 0) -> dict:
    key_list = jax.random.split(jax.random.key(seed), 15)
    part_keys = jax.random.split(jax.random.fold_in(key_list[14], part), 15)
    tokens = draw_tokens(jax.random.fold_in(jax.random.fold_in(key_list[14], part), 71), part)
    gain = jnp.clip(1.0 + 0.18 * jax.random.normal(key_list[1], (D,), jnp.float32), 0.1, 1.9)
    w_query = draw_w_query(jax.random.fold_in(key_list[14], 71), part)
    w_key = draw_w_key(jax.random.fold_in(key_list[14], 71), part)
    w_value = centred(key_list[4], (D, KVW), D ** -0.5, 0.125, ((0, 8), (1, 2)))
    w_input = centred(key_list[5], (D, CW), D ** -0.5, 0.125, ((0, 8), (1, 2)))
    w_bgate = centred(key_list[6], (D, CW), D ** -0.5, 0.125, ((0, 8), (1, 2)))
    w_cgate = centred(key_list[7], (D, CW), D ** -0.5, 0.125, ((0, 8), (1, 2)))
    w_attn_out = centred(key_list[8], (QW, D), (max(1, QW // 128)) ** -0.5, 2.0, ((0, 8), (1, 2)))
    w_conv_out = centred(key_list[9], (CW, D), CW ** -0.5, 0.1875, ((0, 8), (1, 2)))
    sink_logit = jnp.clip(5.0 * jax.random.uniform(key_list[10], (Q_HEADS,), jnp.float32) ** steps_of(key_list[10], (Q_HEADS,), ((0, 2),), -0.2, 0.2), 0.0, 5.0)
    taps = centred(key_list[11], (3, CW), 3 ** -0.5, 3.5, ((1, 2),), jnp.float32)
    conv_bias = centred(key_list[12], (CW,), 1.0, 4.0, ((0, 2),), jnp.float32)
    documents = jnp.searchsorted(jnp.cumsum(uneven(part_keys[13], DOCS, TOKENS, 4 * TOK_DEV, 0)), jnp.arange(TOKENS), side="right").astype(jnp.int32)
    return {"tokens": tokens, "gain": gain, "w_query": w_query, "w_key": w_key, "w_value": w_value, "w_input": w_input, "w_bgate": w_bgate, "w_cgate": w_cgate, "w_attn_out": w_attn_out, "w_conv_out": w_conv_out, "sink_logit": sink_logit, "taps": taps, "conv_bias": conv_bias, "documents": documents}


EPS = 1e-06
THETA = 500000.0

def rotate(proj, positions, heads):
    rows = proj.shape[0]
    size = proj.shape[1] // heads
    half = size // 2
    freq = jnp.power(THETA, -(jnp.arange(half, dtype=jnp.float32) * (2.0 / size)))
    angle = positions.astype(jnp.float32)[:, None] * freq[None, :]
    cosine = jnp.cos(angle)[:, None, :]
    sine = jnp.sin(angle)[:, None, :]
    shaped = proj.reshape(rows, heads, size)
    first = shaped[..., :half]
    second = shaped[..., half:]
    turned = jnp.concatenate([first * cosine - second * sine, second * cosine + first * sine], axis=-1)
    return turned.reshape(rows, heads * size)

def sink_softmax(scores, allowed, sinks):
    masked = jnp.where(allowed, scores, -jnp.inf)
    top = jnp.maximum(lax.optimization_barrier(jnp.max(masked, axis=-1, keepdims=True)), sinks)
    expo = jnp.exp(masked - top)
    return expo / (lax.optimization_barrier(jnp.sum(expo, axis=-1, keepdims=True)) + jnp.exp(sinks - top))

def reference(tokens, gain, w_query, w_key, w_value, w_input, w_bgate, w_cgate, w_attn_out, w_conv_out, sink_logit, taps, conv_bias, documents):
    f32 = jnp.float32
    total = tokens.shape[0]
    xf = tokens.astype(f32)
    inv = lax.rsqrt(lax.optimization_barrier(jnp.sum(xf * xf, axis=1)) / D + EPS)[:, None]
    scaled = (xf * gain[None, :]).astype(jnp.bfloat16)
    qp = jnp.dot(scaled, w_query, preferred_element_type=f32) * inv
    kp = jnp.dot(scaled, w_key, preferred_element_type=f32) * inv
    vp = jnp.dot(scaled, w_value, preferred_element_type=f32) * inv
    upr = jnp.dot(scaled, w_input, preferred_element_type=f32) * inv
    bpr = jnp.dot(scaled, w_bgate, preferred_element_type=f32) * inv
    cpr = jnp.dot(scaled, w_cgate, preferred_element_type=f32) * inv
    positions = jnp.arange(total, dtype=jnp.int32)
    query = rotate(qp, positions, Q_HEADS).astype(jnp.bfloat16)
    keys = rotate(kp, positions, KV_HEADS).astype(jnp.bfloat16).reshape(total, KV_HEADS, HEAD_DIM)
    values = vp.astype(jnp.bfloat16).reshape(total, KV_HEADS, HEAD_DIM)
    groups = Q_HEADS // KV_HEADS
    sinks = sink_logit.astype(f32).reshape(KV_HEADS, groups, 1, 1)
    key_pad = jnp.pad(keys, ((WINDOW, WINDOW), (0, 0), (0, 0)))
    val_pad = jnp.pad(values, ((WINDOW, WINDOW), (0, 0), (0, 0)))
    doc_pad = jnp.pad(documents, (WINDOW, WINDOW), constant_values=-1)
    block = math.gcd(total, 512)
    span = block + 2 * WINDOW

    def one_block(index):
        begin = (index * block).astype(jnp.int32)
        qb = lax.dynamic_slice_in_dim(query, begin, block, 0).reshape(block, KV_HEADS, groups, HEAD_DIM)
        kb = lax.dynamic_slice_in_dim(key_pad, begin, span, 0)
        vb = lax.dynamic_slice_in_dim(val_pad, begin, span, 0)
        qdoc = lax.dynamic_slice_in_dim(documents, begin, block, 0)
        kdoc = lax.dynamic_slice_in_dim(doc_pad, begin, span, 0)
        qpos = begin + jnp.arange(block, dtype=jnp.int32)
        kpos = begin - WINDOW + jnp.arange(span, dtype=jnp.int32)
        scores = jnp.einsum('qhgd,khd->hgqk', qb.astype(f32), kb.astype(f32)) * HEAD_DIM ** (-0.5)
        allowed = (jnp.abs(qpos[:, None] - kpos[None, :]) <= WINDOW) & (qdoc[:, None] == kdoc[None, :])
        allowed = allowed & (kpos >= 0)[None, :] & (kpos < total)[None, :]
        weight = sink_softmax(scores, allowed, sinks).astype(jnp.bfloat16)
        out = jnp.einsum('hgqk,khd->qhgd', weight.astype(f32), vb.astype(f32))
        return out.astype(jnp.bfloat16).reshape(block, Q_HEADS * HEAD_DIM)
    attended = lax.map(one_block, jnp.arange(total // block, dtype=jnp.int32)).reshape(total, Q_HEADS * HEAD_DIM)
    carried = (cpr * upr).astype(jnp.bfloat16)
    car_pad = jnp.pad(carried, ((1, 1), (0, 0)))
    doc_near = jnp.pad(documents, (1, 1), constant_values=-1)
    conv = jnp.zeros((total, CW), f32)
    for tap in range(3):
        same = (doc_near[tap:tap + total] == documents)[:, None]
        conv = conv + jnp.where(same, car_pad[tap:tap + total].astype(f32) * taps[tap][None, :], 0.0)
    convolved = (bpr * (conv + conv_bias[None, :])).astype(jnp.bfloat16)
    mixed = jnp.dot(attended, w_attn_out, preferred_element_type=f32) + jnp.dot(convolved, w_conv_out, preferred_element_type=f32)
    return mixed.astype(jnp.bfloat16)
```

```python
import functools

import jax
import jax.numpy as jnp
from jax import lax
from jax.experimental import pallas as pl
from jax.experimental.pallas import tpu as pltpu
from jax.sharding import PartitionSpec as P

HEAD_DIM = 64
WINDOW = 128


EPS = 1e-06
THETA = 500000.0
PROJ_UNITS = 4
OUT_UNITS = 2
TOKEN_CHUNKS = 4


def fused_plan(grp_count, sp_count, tp_count, rows, part, proj_rows, out_rows):
    lines = sp_count // 2
    return (
        grp_count == 2
        and tp_count == 2
        and sp_count % 2 == 0
        and 2 <= lines <= 4
        and proj_rows % (2 * PROJ_UNITS * 16) == 0
        and out_rows % (2 * OUT_UNITS * 16) == 0
        and rows % (TOKEN_CHUNKS * 16) == 0
        and part % 128 == 0
    )


def gather_kernel(
    sizes,
    tok_ref,
    gain_ref,
    wp_ref,
    wo_ref,
    proj_ref,
    wo_full,
    wp_full,
    tok_other,
    scaled,
    inv_ref,
    z_send,
    z_recv,
    y_send,
    y_recv,
    dz_send,
    dz_recv,
    dy_send,
    dy_recv,
    do_send,
    do_recv,
    x_send,
    x_recv,
    own_sem,
):
    lines, cut = sizes
    f32 = jnp.float32
    rows, part = tok_ref.shape
    rp = wp_ref.shape[0]
    ro = wo_ref.shape[0]
    up, uo = rp // 2 // PROJ_UNITS, ro // 2 // OUT_UNITS
    y = lax.axis_index("grp")
    sp = lax.axis_index("sp")
    x = lax.axis_index("tp")
    z, c = sp // 2, sp % 2
    proj_units = list(range(PROJ_UNITS))
    out_units = list(range(PROJ_UNITS, PROJ_UNITS + OUT_UNITS))
    to_y = {"grp": 1 - y}
    to_core = {"sp": z * 2 + 1 - c}
    to_x = {"tp": 1 - x}
    to_z = ({"sp": sp + 2}, {"sp": sp - 2})
    has_next = (z < lines - 1, z > 0)

    def origin(way, t):
        return z - t if way == 0 else z + t

    def arrives(way, t):
        return z >= t if way == 0 else z < lines - t

    def place(u, zo, cc, h):
        if u < PROJ_UNITS:
            row = (zo * 2 + cc) * rp + h * (rp // 2) + u * up
            return wp_full.at[pl.ds(pl.multiple_of(row, up), up), :]
        row = (zo * 2 + cc) * ro + h * (ro // 2) + (u - PROJ_UNITS) * uo
        return wo_full.at[pl.ds(pl.multiple_of(row, uo), uo), :]

    def mine(u, h):
        if u < PROJ_UNITS:
            row = h * (rp // 2) + u * up
            return wp_ref.at[pl.ds(pl.multiple_of(row, up), up), :]
        row = h * (ro // 2) + (u - PROJ_UNITS) * uo
        return wo_ref.at[pl.ds(pl.multiple_of(row, uo), uo), :]

    def remote(src, dst, send, recv, device):
        return pltpu.make_async_remote_copy(
            src_ref=src, dst_ref=dst, send_sem=send, recv_sem=recv,
            device_id=device, device_id_type=pl.DeviceIdType.MESH,
        )

    def z_copy(way, t, u):
        zo = origin(way, t)
        dst = place(u, zo, c, y)
        src = mine(u, y) if t == 0 else dst
        return remote(src, dst, z_send.at[way, t, u], z_recv.at[way, t, u], to_z[way])

    def z_arrival(way, t, u):
        dst = place(u, origin(way, t), c, y)
        return remote(dst, dst, z_send.at[way, t - 1, u], z_recv.at[way, t - 1, u], to_z[way])

    def y_copy(way, t, u):
        ref = place(u, origin(way, t), c, y)
        return remote(ref, ref, y_send.at[way, t - 1, u], y_recv.at[way, t - 1, u], to_y)

    def y_arrival(way, t, u):
        ref = place(u, origin(way, t), c, 1 - y)
        return remote(ref, ref, y_send.at[way, t - 1, u], y_recv.at[way, t - 1, u], to_y)

    def d_copy(kind, way, t, u, cc):
        send, recv = (dz_send, dz_recv) if kind == 0 else (dy_send, dy_recv)
        ref = place(u, origin(way, t), cc, y if kind == 0 else 1 - y)
        return remote(ref, ref, send.at[way, t - 1, u], recv.at[way, t - 1, u], to_core)

    def own_d(group, cc):
        ref, full, size = (wp_ref, wp_full, rp) if group == 0 else (wo_ref, wo_full, ro)
        dst = full.at[pl.ds(pl.multiple_of((z * 2 + cc) * size, size), size), :]
        return remote(ref, dst, do_send.at[group], do_recv.at[group], to_core)

    def own_local(group):
        ref, full, size = (wp_ref, wp_full, rp) if group == 0 else (wo_ref, wo_full, ro)
        dst = full.at[pl.ds(pl.multiple_of((z * 2 + c) * size, size), size), :]
        return pltpu.make_async_copy(ref, dst, own_sem.at[group])

    chunk = rows // TOKEN_CHUNKS

    def x_copy(k):
        return remote(
            tok_ref.at[pl.ds(k * chunk, chunk), :], tok_other.at[pl.ds(k * chunk, chunk), :],
            x_send.at[k], x_recv.at[k], to_x,
        )

    barrier = pltpu.get_barrier_semaphore()
    for device in (to_y, to_core, to_x):
        pl.semaphore_signal(barrier, inc=1, device_id=device, device_id_type=pl.DeviceIdType.MESH)
    for way in range(2):

        @pl.when(has_next[way])
        def _():
            pl.semaphore_signal(
                barrier, inc=1, device_id=to_z[way], device_id_type=pl.DeviceIdType.MESH
            )

    neighbours = jnp.where(z > 0, 1, 0) + jnp.where(z < lines - 1, 1, 0) + 3
    pl.semaphore_wait(barrier, neighbours)

    def start_own(units):
        for u in units:
            for way in range(2):

                @pl.when(has_next[way])
                def _():
                    z_copy(way, 0, u).start()

    start_own(proj_units)
    for k in range(TOKEN_CHUNKS):
        x_copy(k).start()
    own_d(0, c).start()
    own_local(0).start()

    def event(t, u):
        for way in range(2):

            @pl.when(arrives(way, t))
            def _():
                z_arrival(way, t, u).wait_recv()
                if t < lines - 1:

                    @pl.when(has_next[way])
                    def _():
                        z_copy(way, t, u).start()

                y_copy(way, t, u).start()
                d_copy(0, way, t, u, c).start()

    def y_event(t, u):
        for way in range(2):

            @pl.when(arrives(way, t))
            def _():
                y_arrival(way, t, u).wait_recv()
                d_copy(1, way, t, u, c).start()

    def scale(k):
        x_copy(k).wait_recv()
        tile = 32

        def body(i, carry):
            at = pl.ds(pl.multiple_of(k * chunk + i * tile, tile), tile)
            own = tok_ref[at, :].astype(f32)
            other = tok_other[at, :].astype(f32)
            total = jnp.sum(own * own, axis=1, keepdims=True) + jnp.sum(
                other * other, axis=1, keepdims=True
            )
            inv_ref[at, :] = jnp.broadcast_to(
                lax.rsqrt(total / (2 * part) + EPS), (tile, inv_ref.shape[1])
            )
            mine_at = pl.multiple_of(x * part, part)
            other_at = pl.multiple_of((1 - x) * part, part)
            scaled[at, pl.ds(mine_at, part)] = (own * gain_ref[:, pl.ds(mine_at, part)]).astype(
                scaled.dtype
            )
            scaled[at, pl.ds(other_at, part)] = (
                other * gain_ref[:, pl.ds(other_at, part)]
            ).astype(scaled.dtype)
            return carry

        lax.fori_loop(0, chunk // tile, body, 0)

    steps = [(t, u) for t in range(1, lines) for u in proj_units]
    done = 0
    for i, (t, u) in enumerate(steps):
        event(t, u)
        if i >= 1:
            y_event(*steps[i - 1])
        if (t, u) == (lines - 1, 0):
            start_own(out_units)
            own_d(1, c).start()
            own_local(1).start()
        while done < TOKEN_CHUNKS - 1 and (i + 1) * TOKEN_CHUNKS >= (done + 1) * len(steps):
            scale(done)
            done += 1
    y_event(*steps[-1])
    while done < TOKEN_CHUNKS:
        scale(done)
        done += 1
    own_d(0, 1 - c).wait_recv()
    own_local(0).wait()
    for t, u in steps:
        for way in range(2):

            @pl.when(arrives(way, t))
            def _():
                d_copy(0, way, t, u, 1 - c).wait_recv()
                d_copy(1, way, t, u, 1 - c).wait_recv()

    width = proj_ref.shape[1]
    blocks = width // cut
    tail = [(t, u) for t in range(1, lines) for u in out_units]
    cuts = [blocks * i // len(tail) for i in range(len(tail) + 1)]

    def project(begin, end):
        def body(j, carry):
            at = pl.ds(pl.multiple_of(j * cut, cut), cut)
            acc = jnp.dot(scaled[...], wp_full[:, at], preferred_element_type=f32)
            proj_ref[:, at] = acc * inv_ref[:, :1]
            return carry

        lax.fori_loop(begin, end, body, 0)

    for i, (t, u) in enumerate(tail):
        project(cuts[i], cuts[i + 1])
        event(t, u)
        if i >= 1:
            y_event(*tail[i - 1])
    y_event(*tail[-1])
    own_d(1, 1 - c).wait_recv()
    own_local(1).wait()
    for t, u in tail:
        for way in range(2):

            @pl.when(arrives(way, t))
            def _():
                d_copy(0, way, t, u, 1 - c).wait_recv()
                d_copy(1, way, t, u, 1 - c).wait_recv()

    for group in range(2):
        own_d(group, c).wait_send()
    for k in range(TOKEN_CHUNKS):
        x_copy(k).wait_send()
    for u in proj_units + out_units:
        for way in range(2):

            @pl.when(has_next[way])
            def _():
                z_copy(way, 0, u).wait_send()

            for t in range(1, lines):

                @pl.when(arrives(way, t))
                def _():
                    if t < lines - 1:

                        @pl.when(has_next[way])
                        def _():
                            z_copy(way, t, u).wait_send()

                    y_copy(way, t, u).wait_send()
                    d_copy(0, way, t, u, c).wait_send()
                    d_copy(1, way, t, u, c).wait_send()


def gather_project(tokens, gain, w_proj, w_out, sp_count):
    rows, part = tokens.shape
    lines = sp_count // 2
    width = w_proj.shape[1]
    cut = 256 if width % 256 == 0 else 128
    units = PROJ_UNITS + OUT_UNITS
    dma = pltpu.SemaphoreType.DMA
    hops = (2, lines - 1, units)
    vmem = pl.BlockSpec(memory_space=pltpu.VMEM)
    flops = 2 * rows * 2 * part * width
    return pl.pallas_call(
        functools.partial(gather_kernel, (lines, cut)),
        out_shape=(
            jax.ShapeDtypeStruct((rows, width), jnp.float32),
            jax.ShapeDtypeStruct((w_out.shape[0] * sp_count, w_out.shape[1]), w_out.dtype),
        ),
        in_specs=[vmem] * 4,
        out_specs=(vmem, pl.BlockSpec(memory_space=pl.ANY)),
        scratch_shapes=[
            pltpu.VMEM((w_proj.shape[0] * sp_count, width), w_proj.dtype),
            pltpu.VMEM((rows, part), tokens.dtype),
            pltpu.VMEM((rows, 2 * part), jnp.bfloat16),
            pltpu.VMEM((rows, 128), jnp.float32),
        ]
        + [dma(hops)] * 8
        + [dma((2,)), dma((2,)), dma((TOKEN_CHUNKS,)), dma((TOKEN_CHUNKS,)), dma((2,))],
        compiler_params=pltpu.CompilerParams(
            collective_id=0, has_side_effects=True, vmem_limit_bytes=60 * 1024 * 1024
        ),
        cost_estimate=pl.CostEstimate(flops=flops, bytes_accessed=0, transcendentals=0),
        name="gather_project",
    )(tokens, gain[None, :], w_proj, w_out)


def extended(cells, sides, width):
    for axis, dim in sides:
        count = lax.axis_size(axis)
        ends = count - 1
        head = lax.slice_in_dim(cells, 0, width, axis=dim)
        tail = lax.slice_in_dim(cells, cells.shape[dim] - width, cells.shape[dim], axis=dim)
        cells = jnp.concatenate(
            [
                lax.ppermute(tail, axis, [(i, (i + 1) % count) for i in range(ends)]),
                cells,
                lax.ppermute(head, axis, [((i + 1) % count, i) for i in range(ends)]),
            ],
            axis=dim,
        )
    return cells


def rotate(proj, positions, heads):
    rows = proj.shape[0]
    size = proj.shape[1] // heads
    half = size // 2
    freq = jnp.power(THETA, -(jnp.arange(half, dtype=jnp.float32) * (2.0 / size)))
    angle = positions.astype(jnp.float32)[:, None] * freq[None, :]
    cosine = jnp.cos(angle)[:, None, :]
    sine = jnp.sin(angle)[:, None, :]
    shaped = proj.reshape(rows, heads, size)
    first = shaped[..., :half]
    second = shaped[..., half:]
    turned = jnp.concatenate(
        [first * cosine - second * sine, second * cosine + first * sine], axis=-1
    )
    return turned.reshape(rows, heads * size)


def sink_softmax(scores, allowed, sinks):
    masked = jnp.where(allowed, scores, -jnp.inf)
    top = jnp.maximum(jnp.max(masked, axis=-1, keepdims=True), sinks)
    expo = jnp.exp(masked - top)
    return expo / (jnp.sum(expo, axis=-1, keepdims=True) + jnp.exp(sinks - top))


def local(
    tokens,
    gain,
    w_query,
    w_key,
    w_value,
    w_input,
    w_bgate,
    w_cgate,
    w_attn_out,
    w_conv_out,
    sink_logit,
    taps,
    conv_bias,
    documents,
):
    f32 = jnp.float32
    bf16 = jnp.bfloat16
    rows, part = tokens.shape
    tp_count = lax.axis_size("tp")
    sp_count = lax.axis_size("sp")
    width = part * tp_count
    head_dim = HEAD_DIM
    q_local = w_query.shape[1] // head_dim
    kv_local = w_key.shape[1] // head_dim
    groups = q_local // kv_local
    if fused_plan(
        lax.axis_size("grp"), sp_count, tp_count, rows, part, w_query.shape[0], w_attn_out.shape[0]
    ):
        cols = (w_query, w_key, w_value, w_input, w_bgate, w_cgate)
        proj, w_both = gather_project(
            tokens,
            gain,
            jnp.concatenate(cols, axis=1),
            jnp.concatenate((w_attn_out, w_conv_out), axis=1),
            sp_count,
        )
        parts, at = [], 0
        for col in cols:
            parts.append(proj[:, at : at + col.shape[1]])
            at += col.shape[1]
        q_acc, k_acc, v_acc, u_acc, b_acc, c_acc = parts
        w_attn = w_both[:, :part]
        w_conv = w_both[:, part:]
        inv = jnp.float32(1.0)
    else:
        wq, wk, wv, wu, wb, wc, w_attn, w_conv = (
            lax.all_gather(w_query, "sp", axis=0, tiled=True),
            lax.all_gather(w_key, "sp", axis=0, tiled=True),
            lax.all_gather(w_value, "sp", axis=0, tiled=True),
            lax.all_gather(w_input, "sp", axis=0, tiled=True),
            lax.all_gather(w_bgate, "sp", axis=0, tiled=True),
            lax.all_gather(w_cgate, "sp", axis=0, tiled=True),
            lax.all_gather(w_attn_out, "sp", axis=0, tiled=True),
            lax.all_gather(w_conv_out, "sp", axis=0, tiled=True),
        )
        matrices = (wq, wk, wv, wu, wb, wc)
        piece_f = lax.all_gather(tokens, "tp", axis=1, tiled=True).astype(f32)
        scaled = (piece_f * gain[None, :]).astype(bf16)
        products = tuple((jnp.dot(scaled, mat, preferred_element_type=f32) for mat in matrices))
        folded = products + (jnp.sum(piece_f * piece_f, axis=1),)
        sums = folded[:6]
        squares = folded[6]
        inv = lax.rsqrt(squares / width + EPS)[:, None]
        q_acc, k_acc, v_acc, u_acc, b_acc, c_acc = sums
    positions = lax.axis_index("sp") * rows + jnp.arange(rows, dtype=jnp.int32)
    query = rotate(q_acc * inv, positions, q_local).astype(bf16)
    keys = rotate(k_acc * inv, positions, kv_local).astype(bf16)
    values = (v_acc * inv).astype(bf16)
    carried = (c_acc * inv * (u_acc * inv)).astype(bf16)
    bgate = b_acc * inv
    doc_col = documents.astype(f32).astype(bf16)[:, None]
    paired = jnp.concatenate([keys, values], axis=1)
    pair_ext, doc_ext = (
        extended(paired, (("sp", 0),), WINDOW),
        extended(doc_col, (("sp", 0),), WINDOW),
    )
    carry_ext, doc_near = (extended(carried, (("sp", 0),), 1), extended(doc_col, (("sp", 0),), 1))
    key_width = kv_local * head_dim
    key_ext = pair_ext[:, :key_width].reshape(-1, kv_local, head_dim)
    val_ext = pair_ext[:, key_width:].reshape(-1, kv_local, head_dim)
    key_doc = doc_ext[:, 0].astype(f32)
    own_doc = doc_col[:, 0].astype(f32)
    key_pos = positions[0] - WINDOW + jnp.arange(rows + 2 * WINDOW, dtype=jnp.int32)
    total = sp_count * rows
    sinks = sink_logit.reshape(kv_local, groups, 1, 1)
    block = rows // 2
    outputs = []
    for begin in range(0, rows, block):
        span = block + 2 * WINDOW
        q_block = query[begin : begin + block].reshape(block, kv_local, groups, head_dim)
        k_block = key_ext[begin : begin + span]
        v_block = val_ext[begin : begin + span]
        q_pos = positions[begin : begin + block]
        k_pos = key_pos[begin : begin + span]
        scores = jnp.einsum(
            "qhgd,khd->hgqk", q_block, k_block, preferred_element_type=f32
        ) * head_dim ** (-0.5)
        allowed = jnp.abs(q_pos[:, None] - k_pos[None, :]) <= WINDOW
        allowed = allowed & (
            own_doc[begin : begin + block, None] == key_doc[None, begin : begin + span]
        )
        allowed = allowed & (k_pos >= 0)[None, :] & (k_pos < total)[None, :]
        weight = sink_softmax(scores, allowed, sinks).astype(bf16)
        result = jnp.einsum("hgqk,khd->qhgd", weight, v_block, preferred_element_type=f32)
        outputs.append(result.astype(bf16).reshape(block, q_local * head_dim))
    attended = jnp.concatenate(outputs, axis=0)
    near_doc = doc_near[:, 0].astype(f32)
    conv = jnp.zeros((rows, carried.shape[1]), f32)
    for tap in range(3):
        same = (near_doc[tap : tap + rows] == near_doc[1 : rows + 1])[:, None]
        conv = conv + jnp.where(
            same, carry_ext[tap : tap + rows].astype(f32) * taps[tap][None, :], 0.0
        )
    convolved = (bgate * (conv + conv_bias[None, :])).astype(bf16)
    me = lax.axis_index("tp")
    terms = []
    for shift in range(tp_count):
        hops = [(i, (i + shift) % tp_count) for i in range(tp_count)]
        owner = (me + tp_count - shift) % tp_count
        for mixer, weight in ((convolved, w_conv), (attended, w_attn)):
            piece = mixer if shift == 0 else lax.ppermute(mixer, "tp", hops)
            span = piece.shape[1]
            terms.append(
                jnp.dot(
                    piece,
                    lax.dynamic_slice_in_dim(weight, owner * span, span, 0),
                    preferred_element_type=f32,
                )
            )
    mixed = functools.reduce(jnp.add, terms)
    return mixed.astype(bf16)


def solution(mesh):
    placed = (
        P(("grp", "sp"), "tp"),
        P(),
        P("sp", "tp"),
        P("sp", "tp"),
        P("sp", "tp"),
        P("sp", "tp"),
        P("sp", "tp"),
        P("sp", "tp"),
        P("sp", "tp"),
        P("sp", "tp"),
        P("tp"),
        P(None, "tp"),
        P("tp"),
        P(("grp", "sp")),
    )
    return jax.shard_map(
        local, mesh=mesh, in_specs=placed, out_specs=P(("grp", "sp"), "tp"), check_vma=False
    )
```

```python
import functools

import jax
import jax.numpy as jnp
from jax import lax
from jax.experimental import pallas as pl
from jax.experimental.pallas import tpu as pltpu
from jax.sharding import PartitionSpec as P

HEAD_DIM = 64
WINDOW = 128


EPS = 1e-06
THETA = 500000.0
PROJ_UNITS = 4
OUT_UNITS = 2
TOKEN_CHUNKS = 4


def fused_plan(grp_count, sp_count, tp_count, rows, part, proj_rows, out_rows, q_width, k_width, c_width):
    lines = sp_count // 2
    return (
        grp_count == 2
        and tp_count == 2
        and sp_count % 2 == 0
        and 2 <= lines <= 4
        and proj_rows % (2 * PROJ_UNITS * 16) == 0
        and out_rows % (2 * OUT_UNITS * 16) == 0
        and rows % (TOKEN_CHUNKS * 16) == 0
        and rows % (2 * WINDOW) == 0
        and part % 256 == 0
        and q_width % 256 == 0
        and k_width == 128
        and c_width % 256 == 0
        and 2 * HEAD_DIM == 128
    )


def layer_kernel(
    sizes,
    tok_ref,
    gain_ref,
    wk_ref,
    wv_ref,
    wc_ref,
    wu_ref,
    wb_ref,
    wq_ref,
    wa_ref,
    wm_ref,
    sink_ref,
    taps_ref,
    bias_ref,
    doc_ref,
    doc_col,
    cos_ref,
    sin_ref,
    out_ref,
    wp_full,
    wo_full,
    tok_other,
    scaled,
    inv_ref,
    proj_ref,
    pair_ext,
    query_s,
    carried,
    carry_near,
    doc_row,
    convolved,
    conv_other,
    attended,
    att_other,
    z_send,
    z_recv,
    y_send,
    y_recv,
    dz_send,
    dz_recv,
    dy_send,
    dy_recv,
    do_send,
    do_recv,
    x_send,
    x_recv,
    own_sem,
    halo_send,
    halo_recv,
    conv_sem,
    att_send,
    att_recv,
):
    lines, rp, ro = sizes
    f32 = jnp.float32
    rows, part = tok_ref.shape
    bf16 = jnp.bfloat16
    up, uo = rp // 2 // PROJ_UNITS, ro // 2 // OUT_UNITS
    y = lax.axis_index("grp")
    sp = lax.axis_index("sp")
    x = lax.axis_index("tp")
    z, c = sp // 2, sp % 2
    proj_units = list(range(PROJ_UNITS))
    out_units = list(range(PROJ_UNITS, PROJ_UNITS + OUT_UNITS))
    to_y = {"grp": 1 - y}
    to_core = {"sp": z * 2 + 1 - c}
    to_x = {"tp": 1 - x}
    to_z = ({"sp": sp + 2}, {"sp": sp - 2})
    has_next = (z < lines - 1, z > 0)

    def origin(way, t):
        return z - t if way == 0 else z + t

    def arrives(way, t):
        return z >= t if way == 0 else z < lines - t

    def place(u, zo, cc, h):
        if u < PROJ_UNITS:
            row = (zo * 2 + cc) * rp + h * (rp // 2) + u * up
            return wp_full.at[pl.ds(pl.multiple_of(row, up), up), :]
        row = (zo * 2 + cc) * ro + h * (ro // 2) + (u - PROJ_UNITS) * uo
        return wo_full.at[pl.ds(pl.multiple_of(row, uo), uo), :]

    def remote(src, dst, send, recv, device):
        return pltpu.make_async_remote_copy(
            src_ref=src, dst_ref=dst, send_sem=send, recv_sem=recv,
            device_id=device, device_id_type=pl.DeviceIdType.MESH,
        )

    def z_copy(way, t, u):
        zo = origin(way, t)
        dst = place(u, zo, c, y)
        return remote(dst, dst, z_send.at[way, t, u], z_recv.at[way, t, u], to_z[way])

    def z_arrival(way, t, u):
        dst = place(u, origin(way, t), c, y)
        return remote(dst, dst, z_send.at[way, t - 1, u], z_recv.at[way, t - 1, u], to_z[way])

    def y_copy(way, t, u):
        ref = place(u, origin(way, t), c, y)
        return remote(ref, ref, y_send.at[way, t - 1, u], y_recv.at[way, t - 1, u], to_y)

    def y_arrival(way, t, u):
        ref = place(u, origin(way, t), c, 1 - y)
        return remote(ref, ref, y_send.at[way, t - 1, u], y_recv.at[way, t - 1, u], to_y)

    def d_copy(kind, way, t, u, cc):
        send, recv = (dz_send, dz_recv) if kind == 0 else (dy_send, dy_recv)
        ref = place(u, origin(way, t), cc, y if kind == 0 else 1 - y)
        return remote(ref, ref, send.at[way, t - 1, u], recv.at[way, t - 1, u], to_core)

    def shard(group, cc):
        full, size = (wp_full, rp) if group == 0 else (wo_full, ro)
        return full, pl.ds(pl.multiple_of((z * 2 + cc) * size, size), size)

    def own_d(group, cc):
        full, at = shard(group, cc)
        dst = full.at[at, :]
        return remote(dst, dst, do_send.at[group], do_recv.at[group], to_core)

    def own_local(group):
        full, at = shard(group, c)
        refs = (wk_ref, wv_ref, wc_ref, wu_ref, wb_ref, wq_ref) if group == 0 else (wa_ref, wm_ref)
        copies, col = [], 0
        for j, ref in enumerate(refs):
            size = ref.shape[1]
            copies.append(
                pltpu.make_async_copy(
                    ref, full.at[at, pl.ds(col, size)], own_sem.at[6 * group + j]
                )
            )
            col += size
        return copies

    chunk = rows // TOKEN_CHUNKS

    def x_copy(k):
        return remote(
            tok_ref.at[pl.ds(k * chunk, chunk), :], tok_other.at[pl.ds(k * chunk, chunk), :],
            x_send.at[k], x_recv.at[k], to_x,
        )

    last = 2 * lines - 1
    steps_sp = (sp + 1, sp - 1)
    sends_to = (sp < last, sp > 0)
    gets_from = (sp > 0, sp < last)
    side = jnp.where(c == 0, sp - 1, sp + 1)
    has_side = (side >= 0) & (side <= last)

    def halo(kind, way):
        if kind == 0:
            src = doc_ref.at[:, rows - WINDOW : rows] if way == 0 else doc_ref.at[:, 0:WINDOW]
            at = 0 if way == 0 else WINDOW + rows
            dst = doc_row.at[:, at : at + WINDOW]
        elif kind == 1:
            at = rows if way == 0 else WINDOW
            src = pair_ext.at[at : at + WINDOW, :]
            at = 0 if way == 0 else WINDOW + rows
            dst = pair_ext.at[at : at + WINDOW, :]
        else:
            at = rows - 16 if way == 0 else 0
            src = carried.at[at : at + 16, :]
            dst = carry_near.at[way]
        return remote(
            src, dst, halo_send.at[kind, way], halo_recv.at[kind, way], {"sp": steps_sp[way]}
        )

    def start_halo(kind):
        for way in range(2):

            @pl.when(sends_to[way])
            def _():
                halo(kind, way).start()

    def wait_halo(kind):
        for way in range(2):

            @pl.when(gets_from[way])
            def _():
                halo(kind, way).wait_recv()

    def conv_copy():
        return remote(convolved, conv_other, conv_sem.at[0], conv_sem.at[1], to_x)

    def att_copy(i):
        at = pl.ds(pl.multiple_of(i * WINDOW, WINDOW), WINDOW)
        return remote(attended.at[at, :], att_other.at[at, :], att_send.at[i], att_recv.at[i], to_x)

    for copy in own_local(0) + own_local(1):
        copy.start()

    barrier = pltpu.get_barrier_semaphore()
    for device in (to_y, to_core, to_x):
        pl.semaphore_signal(barrier, inc=1, device_id=device, device_id_type=pl.DeviceIdType.MESH)
    for way in range(2):

        @pl.when(has_next[way])
        def _():
            pl.semaphore_signal(
                barrier, inc=1, device_id=to_z[way], device_id_type=pl.DeviceIdType.MESH
            )

    @pl.when(has_side)
    def _():
        pl.semaphore_signal(
            barrier, inc=1, device_id={"sp": side}, device_id_type=pl.DeviceIdType.MESH
        )

    neighbours = jnp.where(has_side, 1, 0) + jnp.where(z > 0, 1, 0) + jnp.where(z < lines - 1, 1, 0) + 3
    pl.semaphore_wait(barrier, neighbours)

    def start_own(units):
        for u in units:
            for way in range(2):

                @pl.when(has_next[way])
                def _():
                    z_copy(way, 0, u).start()

    for k in range(TOKEN_CHUNKS):
        x_copy(k).start()
    for copy in own_local(0):
        copy.wait()
    start_own(proj_units)
    own_d(0, c).start()
    start_halo(0)
    doc_row[:, WINDOW : WINDOW + rows] = doc_ref[...]

    @pl.when(sp == 0)
    def _():
        doc_row[:, :WINDOW] = jnp.full((doc_row.shape[0], WINDOW), -1.0, f32)
        pair_ext[:WINDOW, :] = jnp.zeros((WINDOW, pair_ext.shape[1]), bf16)

    @pl.when(sp == last)
    def _():
        doc_row[:, WINDOW + rows :] = jnp.full((doc_row.shape[0], WINDOW), -1.0, f32)
        pair_ext[WINDOW + rows :, :] = jnp.zeros((WINDOW, pair_ext.shape[1]), bf16)


    def event(t, u):
        for way in range(2):

            @pl.when(arrives(way, t))
            def _():
                z_arrival(way, t, u).wait_recv()
                if t < lines - 1:

                    @pl.when(has_next[way])
                    def _():
                        z_copy(way, t, u).start()

                y_copy(way, t, u).start()
                d_copy(0, way, t, u, c).start()

    def y_event(t, u):
        for way in range(2):

            @pl.when(arrives(way, t))
            def _():
                y_arrival(way, t, u).wait_recv()
                d_copy(1, way, t, u, c).start()

    def scale(k):
        x_copy(k).wait_recv()
        tile = 32

        def body(i, carry):
            at = pl.ds(pl.multiple_of(k * chunk + i * tile, tile), tile)
            own = tok_ref[at, :].astype(f32)
            other = tok_other[at, :].astype(f32)
            total = jnp.sum(own * own, axis=1, keepdims=True) + jnp.sum(
                other * other, axis=1, keepdims=True
            )
            inv_ref[at, :] = jnp.broadcast_to(
                lax.rsqrt(total / (2 * part) + EPS), (tile, inv_ref.shape[1])
            )
            mine_at = pl.multiple_of(x * part, part)
            other_at = pl.multiple_of((1 - x) * part, part)
            scaled[at, pl.ds(mine_at, part)] = (own * gain_ref[:, pl.ds(mine_at, part)]).astype(
                scaled.dtype
            )
            scaled[at, pl.ds(other_at, part)] = (
                other * gain_ref[:, pl.ds(other_at, part)]
            ).astype(scaled.dtype)
            return carry

        lax.fori_loop(0, chunk // tile, body, 0)

    steps = [(t, u) for t in range(1, lines) for u in proj_units]
    done = 0
    for i, (t, u) in enumerate(steps):
        event(t, u)
        if i >= 1:
            y_event(*steps[i - 1])
        if (t, u) == (lines - 1, 0):
            for copy in own_local(1):
                copy.wait()
            start_own(out_units)
            own_d(1, c).start()
        while done < TOKEN_CHUNKS - 1 and (i + 1) * TOKEN_CHUNKS >= (done + 1) * len(steps):
            scale(done)
            done += 1
    y_event(*steps[-1])
    while done < TOKEN_CHUNKS:
        scale(done)
        done += 1
    own_d(0, 1 - c).wait_recv()
    for t, u in steps:
        for way in range(2):

            @pl.when(arrives(way, t))
            def _():
                d_copy(0, way, t, u, 1 - c).wait_recv()
                d_copy(1, way, t, u, 1 - c).wait_recv()

    tail = [(t, u) for t in range(1, lines) for u in out_units]
    pending = list(enumerate(tail))
    beats = 6

    def advance(beat):
        goal = len(tail) * (beats - 1 - beat) // beats
        while len(pending) > goal:
            i, (t, u) = pending.pop(0)
            event(t, u)
            if i >= 1:
                y_event(*tail[i - 1])

    cut = 256
    k_width, c_width, q_width = wk_ref.shape[1], wc_ref.shape[1], wq_ref.shape[1]
    c_at = 2 * k_width
    u_at, b_at, q_at = c_at + c_width, c_at + 2 * c_width, c_at + 3 * c_width

    def project(begin, end):
        def body(j, carry):
            at = pl.ds(pl.multiple_of(j * cut, cut), cut)
            acc = jnp.dot(scaled[...], wp_full[:, at], preferred_element_type=f32)
            proj_ref[:, at] = acc * inv_ref[:, :1]
            return carry

        lax.fori_loop(begin // cut, end // cut, body, 0)

    lanes = 128
    lane = lax.broadcasted_iota(jnp.int32, (rows, lanes), 1)
    low = (lane % HEAD_DIM) < HEAD_DIM // 2

    def turned(cells):
        ahead = pltpu.roll(cells, lanes - HEAD_DIM // 2, 1)
        behind = pltpu.roll(cells, HEAD_DIM // 2, 1)
        return cells * cos_ref[...] + jnp.where(low, ahead, behind) * sin_ref[...]

    def block(at, j):
        return pl.ds(pl.multiple_of(at + j * lanes, lanes), lanes)

    project(0, c_at)
    pair_ext[WINDOW : WINDOW + rows, :k_width] = turned(proj_ref[:, :k_width]).astype(bf16)
    pair_ext[WINDOW : WINDOW + rows, k_width:] = proj_ref[:, k_width : 2 * k_width].astype(bf16)
    advance(0)
    start_halo(1)
    project(c_at, b_at)

    def carry_body(j, carry):
        carried[:, block(0, j)] = (
            proj_ref[:, block(c_at, j)] * proj_ref[:, block(u_at, j)]
        ).astype(bf16)
        return carry

    lax.fori_loop(0, c_width // lanes, carry_body, 0)
    advance(1)
    start_halo(2)
    project(b_at, q_at)
    advance(2)
    wait_halo(0)
    wait_halo(2)

    row = lax.broadcasted_iota(jnp.int32, (rows, lanes), 0)

    def conv_body(j, carry):
        at = block(0, j)
        docs = doc_col[...]
        cells = carried[:, at].astype(f32)
        before = jnp.where(row == 0, carry_near[0, 15:16, at].astype(f32), pltpu.roll(cells, 1, 0))
        after = jnp.where(
            row == rows - 1, carry_near[1, 0:1, at].astype(f32), pltpu.roll(cells, rows - 1, 0)
        )
        doc_before = jnp.where(row == 0, doc_row[0:1, WINDOW - 1 : WINDOW], pltpu.roll(docs, 1, 0))
        doc_after = jnp.where(
            row == rows - 1,
            doc_row[0:1, WINDOW + rows : WINDOW + rows + 1],
            pltpu.roll(docs, rows - 1, 0),
        )
        conv = jnp.where(doc_before == docs, before * taps_ref[0:1, at], 0.0)
        conv = conv + cells * taps_ref[1:2, at]
        conv = conv + jnp.where(doc_after == docs, after * taps_ref[2:3, at], 0.0)
        convolved[:, at] = (proj_ref[:, block(b_at, j)] * (conv + bias_ref[:, at])).astype(bf16)
        return carry

    lax.fori_loop(0, c_width // lanes, conv_body, 0)
    project(q_at, q_at + q_width)
    conv_copy().start()
    advance(3)

    def query_body(j, carry):
        cells = turned(proj_ref[:, block(q_at, j)])
        query_s[:, block(0, j)] = (cells * HEAD_DIM ** (-0.5)).astype(bf16)
        return carry

    lax.fori_loop(0, q_width // lanes, query_body, 0)
    wait_halo(1)
    kv_heads = k_width // HEAD_DIM
    groups = q_width // HEAD_DIM // kv_heads
    span = 3 * WINDOW
    gap = lax.broadcasted_iota(jnp.int32, (WINDOW, span), 1) - lax.broadcasted_iota(
        jnp.int32, (WINDOW, span), 0
    )
    window = (gap >= 0) & (gap <= 2 * WINDOW)

    def attend(i, carry):
        at = pl.ds(pl.multiple_of(i * WINDOW, WINDOW), WINDOW)
        near = pl.ds(pl.multiple_of(i * WINDOW, WINDOW), span)
        allowed = window & (doc_col[at, 0:1] == doc_row[0:1, near])
        bias = jnp.where(allowed, 0.0, -jnp.inf)
        bias = jnp.concatenate([bias] * groups, axis=0)
        queries = query_s[at, :]
        pairs = pair_ext[near, :]
        for head in range(kv_heads):
            keys = pairs[:, head * HEAD_DIM : (head + 1) * HEAD_DIM]
            values = pairs[:, k_width + head * HEAD_DIM : k_width + (head + 1) * HEAD_DIM]
            first = head * groups
            stack = jnp.concatenate(
                [
                    queries[:, (first + g) * HEAD_DIM : (first + g + 1) * HEAD_DIM]
                    for g in range(groups)
                ],
                axis=0,
            )
            sinks = jnp.concatenate(
                [jnp.full((WINDOW, 1), sink_ref[first + g], f32) for g in range(groups)], axis=0
            )
            scores = lax.dot_general(
                stack, keys, (((1,), (1,)), ((), ())), preferred_element_type=f32
            )
            scores = scores + bias
            top = jnp.maximum(jnp.max(scores, axis=1, keepdims=True), sinks)
            expo = jnp.exp(scores - top)
            total = jnp.sum(expo, axis=1, keepdims=True) + jnp.exp(sinks - top)
            weight = (expo * (1.0 / total)).astype(bf16)
            result = jnp.dot(weight, values, preferred_element_type=f32).astype(bf16)
            wide = jnp.concatenate(
                [result[g * WINDOW : (g + 1) * WINDOW] for g in range(groups)], axis=1
            )
            attended[at, first * HEAD_DIM : (first + groups) * HEAD_DIM] = wide

        @pl.when(i > 0)
        def _():
            att_copy(i - 1).start()

        return carry

    blocks = rows // WINDOW
    lax.fori_loop(0, blocks // 2, attend, 0)
    advance(4)
    lax.fori_loop(blocks // 2, blocks, attend, 0)
    advance(5)
    att_copy(blocks - 1).start()
    y_event(*tail[-1])
    own_d(1, 1 - c).wait_recv()
    for t, u in tail:
        for way in range(2):

            @pl.when(arrives(way, t))
            def _():
                d_copy(0, way, t, u, 1 - c).wait_recv()
                d_copy(1, way, t, u, 1 - c).wait_recv()

    conv_copy().wait_recv()
    q_mine = pl.ds(pl.multiple_of(x * q_width, q_width), q_width)
    q_yours = pl.ds(pl.multiple_of((1 - x) * q_width, q_width), q_width)
    c_mine = pl.ds(pl.multiple_of(x * c_width, c_width), c_width)
    c_yours = pl.ds(pl.multiple_of((1 - x) * c_width, c_width), c_width)

    def mix_body(j, carry):
        at = pl.ds(pl.multiple_of(j * cut, cut), cut)
        late = pl.ds(pl.multiple_of(part + j * cut, cut), cut)
        acc = jnp.dot(attended[...], wo_full[q_mine, at], preferred_element_type=f32)
        acc = acc + jnp.dot(convolved[...], wo_full[c_mine, late], preferred_element_type=f32)
        acc = acc + jnp.dot(conv_other[...], wo_full[c_yours, late], preferred_element_type=f32)
        proj_ref[:, at] = acc
        return carry

    lax.fori_loop(0, part // cut, mix_body, 0)
    half = rows // 2
    for k in range(2):
        for i in range(k * blocks // 2, (k + 1) * blocks // 2):
            att_copy(i).wait_recv()

        def last_body(j, carry):
            at = pl.ds(pl.multiple_of(j * cut, cut), cut)
            acc = proj_ref[k * half : (k + 1) * half, at] + jnp.dot(
                att_other[k * half : (k + 1) * half, :],
                wo_full[q_yours, at],
                preferred_element_type=f32,
            )
            out_ref[k * half : (k + 1) * half, at] = acc.astype(bf16)
            return carry

        lax.fori_loop(0, part // cut, last_body, 0)

    for kind in range(3):
        for way in range(2):

            @pl.when(sends_to[way])
            def _():
                halo(kind, way).wait_send()

    conv_copy().wait_send()
    for i in range(blocks):
        att_copy(i).wait_send()
    for group in range(2):
        own_d(group, c).wait_send()
    for k in range(TOKEN_CHUNKS):
        x_copy(k).wait_send()
    for u in proj_units + out_units:
        for way in range(2):

            @pl.when(has_next[way])
            def _():
                z_copy(way, 0, u).wait_send()

            for t in range(1, lines):

                @pl.when(arrives(way, t))
                def _():
                    if t < lines - 1:

                        @pl.when(has_next[way])
                        def _():
                            z_copy(way, t, u).wait_send()

                    y_copy(way, t, u).wait_send()
                    d_copy(0, way, t, u, c).wait_send()
                    d_copy(1, way, t, u, c).wait_send()


def fused_layer(
    tokens, gain, projections, outputs, sink_logit, taps, conv_bias, documents, sp_count
):
    rows, part = tokens.shape
    f32 = jnp.float32
    bf16 = jnp.bfloat16
    lines = sp_count // 2
    wk, wv, wc, wu, wb, wq = projections
    width = sum(w.shape[1] for w in projections)
    rp, ro = wq.shape[0], outputs[0].shape[0]
    q_width, k_width, c_width = wq.shape[1], wk.shape[1], wc.shape[1]
    half = HEAD_DIM // 2
    lanes = 128
    positions = lax.axis_index("sp") * rows + jnp.arange(rows, dtype=jnp.int32)
    freq = jnp.power(THETA, -(jnp.arange(half, dtype=f32) * (2.0 / HEAD_DIM)))
    angle = positions.astype(f32)[:, None] * freq[None, :]
    cosine, sine = jnp.cos(angle), jnp.sin(angle)
    cosine = jnp.concatenate([cosine] * (lanes // half), axis=1)
    sine = jnp.concatenate([-sine, sine] * (lanes // HEAD_DIM), axis=1)
    docs = documents.astype(f32)
    doc_rows = jnp.broadcast_to(docs[None, :], (8, rows))
    doc_cols = jnp.broadcast_to(docs[:, None], (rows, lanes))
    blocks = rows // WINDOW
    dma = pltpu.SemaphoreType.DMA
    hops = (2, lines - 1, PROJ_UNITS + OUT_UNITS)
    vmem = pl.BlockSpec(memory_space=pltpu.VMEM)
    hbm = pl.BlockSpec(memory_space=pl.ANY)
    smem = pl.BlockSpec(memory_space=pltpu.SMEM)
    flops = 2 * rows * 2 * part * width
    return pl.pallas_call(
        functools.partial(layer_kernel, (lines, rp, ro)),
        out_shape=jax.ShapeDtypeStruct((rows, part), bf16),
        in_specs=[vmem] * 2 + [hbm] * 8 + [smem] + [vmem] * 6,
        out_specs=vmem,
        scratch_shapes=[
            pltpu.VMEM((rp * sp_count, width), bf16),
            pltpu.VMEM((ro * sp_count, 2 * part), bf16),
            pltpu.VMEM((rows, part), bf16),
            pltpu.VMEM((rows, 2 * part), bf16),
            pltpu.VMEM((rows, 128), f32),
            pltpu.VMEM((rows, max(width, part)), f32),
            pltpu.VMEM((rows + 2 * WINDOW, 2 * k_width), bf16),
            pltpu.VMEM((rows, q_width), bf16),
            pltpu.VMEM((rows, c_width), bf16),
            pltpu.VMEM((2, 16, c_width), bf16),
            pltpu.VMEM((8, rows + 2 * WINDOW), f32),
            pltpu.VMEM((rows, c_width), bf16),
            pltpu.VMEM((rows, c_width), bf16),
            pltpu.VMEM((rows, q_width), bf16),
            pltpu.VMEM((rows, q_width), bf16),
        ]
        + [dma(hops)] * 8
        + [dma((2,)), dma((2,)), dma((TOKEN_CHUNKS,)), dma((TOKEN_CHUNKS,)), dma((8,))]
        + [dma((3, 2)), dma((3, 2)), dma((2,)), dma((blocks,)), dma((blocks,))],
        compiler_params=pltpu.CompilerParams(
            collective_id=0, has_side_effects=True, vmem_limit_bytes=62 * 1024 * 1024
        ),
        cost_estimate=pl.CostEstimate(flops=flops, bytes_accessed=0, transcendentals=0),
        name="layer",
    )(
        tokens,
        gain[None, :],
        *projections,
        *outputs,
        sink_logit,
        taps,
        conv_bias[None, :],
        doc_rows,
        doc_cols,
        cosine,
        sine,
    )


def extended(cells, sides, width):
    for axis, dim in sides:
        count = lax.axis_size(axis)
        ends = count - 1
        head = lax.slice_in_dim(cells, 0, width, axis=dim)
        tail = lax.slice_in_dim(cells, cells.shape[dim] - width, cells.shape[dim], axis=dim)
        cells = jnp.concatenate(
            [
                lax.ppermute(tail, axis, [(i, (i + 1) % count) for i in range(ends)]),
                cells,
                lax.ppermute(head, axis, [((i + 1) % count, i) for i in range(ends)]),
            ],
            axis=dim,
        )
    return cells


def rotate(proj, positions, heads):
    rows = proj.shape[0]
    size = proj.shape[1] // heads
    half = size // 2
    freq = jnp.power(THETA, -(jnp.arange(half, dtype=jnp.float32) * (2.0 / size)))
    angle = positions.astype(jnp.float32)[:, None] * freq[None, :]
    cosine = jnp.cos(angle)[:, None, :]
    sine = jnp.sin(angle)[:, None, :]
    shaped = proj.reshape(rows, heads, size)
    first = shaped[..., :half]
    second = shaped[..., half:]
    turned = jnp.concatenate(
        [first * cosine - second * sine, second * cosine + first * sine], axis=-1
    )
    return turned.reshape(rows, heads * size)


def sink_softmax(scores, allowed, sinks):
    masked = jnp.where(allowed, scores, -jnp.inf)
    top = jnp.maximum(jnp.max(masked, axis=-1, keepdims=True), sinks)
    expo = jnp.exp(masked - top)
    return expo / (jnp.sum(expo, axis=-1, keepdims=True) + jnp.exp(sinks - top))


def local(
    tokens,
    gain,
    w_query,
    w_key,
    w_value,
    w_input,
    w_bgate,
    w_cgate,
    w_attn_out,
    w_conv_out,
    sink_logit,
    taps,
    conv_bias,
    documents,
):
    f32 = jnp.float32
    bf16 = jnp.bfloat16
    rows, part = tokens.shape
    tp_count = lax.axis_size("tp")
    sp_count = lax.axis_size("sp")
    width = part * tp_count
    head_dim = HEAD_DIM
    q_local = w_query.shape[1] // head_dim
    kv_local = w_key.shape[1] // head_dim
    groups = q_local // kv_local
    if fused_plan(
        lax.axis_size("grp"),
        sp_count,
        tp_count,
        rows,
        part,
        w_query.shape[0],
        w_attn_out.shape[0],
        w_query.shape[1],
        w_key.shape[1],
        w_input.shape[1],
    ):
        return fused_layer(
            tokens,
            gain,
            (w_key, w_value, w_cgate, w_input, w_bgate, w_query),
            (w_attn_out, w_conv_out),
            sink_logit,
            taps,
            conv_bias,
            documents,
            sp_count,
        )
    wq, wk, wv, wu, wb, wc, w_attn, w_conv = (
        lax.all_gather(w_query, "sp", axis=0, tiled=True),
        lax.all_gather(w_key, "sp", axis=0, tiled=True),
        lax.all_gather(w_value, "sp", axis=0, tiled=True),
        lax.all_gather(w_input, "sp", axis=0, tiled=True),
        lax.all_gather(w_bgate, "sp", axis=0, tiled=True),
        lax.all_gather(w_cgate, "sp", axis=0, tiled=True),
        lax.all_gather(w_attn_out, "sp", axis=0, tiled=True),
        lax.all_gather(w_conv_out, "sp", axis=0, tiled=True),
    )
    matrices = (wq, wk, wv, wu, wb, wc)
    piece_f = lax.all_gather(tokens, "tp", axis=1, tiled=True).astype(f32)
    scaled = (piece_f * gain[None, :]).astype(bf16)
    products = tuple((jnp.dot(scaled, mat, preferred_element_type=f32) for mat in matrices))
    folded = products + (jnp.sum(piece_f * piece_f, axis=1),)
    sums = folded[:6]
    squares = folded[6]
    inv = lax.rsqrt(squares / width + EPS)[:, None]
    q_acc, k_acc, v_acc, u_acc, b_acc, c_acc = sums
    positions = lax.axis_index("sp") * rows + jnp.arange(rows, dtype=jnp.int32)
    query = rotate(q_acc * inv, positions, q_local).astype(bf16)
    keys = rotate(k_acc * inv, positions, kv_local).astype(bf16)
    values = (v_acc * inv).astype(bf16)
    carried = (c_acc * inv * (u_acc * inv)).astype(bf16)
    bgate = b_acc * inv
    doc_col = documents.astype(f32).astype(bf16)[:, None]
    paired = jnp.concatenate([keys, values], axis=1)
    pair_ext, doc_ext = (
        extended(paired, (("sp", 0),), WINDOW),
        extended(doc_col, (("sp", 0),), WINDOW),
    )
    carry_ext, doc_near = (extended(carried, (("sp", 0),), 1), extended(doc_col, (("sp", 0),), 1))
    key_width = kv_local * head_dim
    key_ext = pair_ext[:, :key_width].reshape(-1, kv_local, head_dim)
    val_ext = pair_ext[:, key_width:].reshape(-1, kv_local, head_dim)
    key_doc = doc_ext[:, 0].astype(f32)
    own_doc = doc_col[:, 0].astype(f32)
    key_pos = positions[0] - WINDOW + jnp.arange(rows + 2 * WINDOW, dtype=jnp.int32)
    total = sp_count * rows
    sinks = sink_logit.reshape(kv_local, groups, 1, 1)
    block = rows // 2
    outputs = []
    for begin in range(0, rows, block):
        span = block + 2 * WINDOW
        q_block = query[begin : begin + block].reshape(block, kv_local, groups, head_dim)
        k_block = key_ext[begin : begin + span]
        v_block = val_ext[begin : begin + span]
        q_pos = positions[begin : begin + block]
        k_pos = key_pos[begin : begin + span]
        scores = jnp.einsum(
            "qhgd,khd->hgqk", q_block, k_block, preferred_element_type=f32
        ) * head_dim ** (-0.5)
        allowed = jnp.abs(q_pos[:, None] - k_pos[None, :]) <= WINDOW
        allowed = allowed & (
            own_doc[begin : begin + block, None] == key_doc[None, begin : begin + span]
        )
        allowed = allowed & (k_pos >= 0)[None, :] & (k_pos < total)[None, :]
        weight = sink_softmax(scores, allowed, sinks).astype(bf16)
        result = jnp.einsum("hgqk,khd->qhgd", weight, v_block, preferred_element_type=f32)
        outputs.append(result.astype(bf16).reshape(block, q_local * head_dim))
    attended = jnp.concatenate(outputs, axis=0)
    near_doc = doc_near[:, 0].astype(f32)
    conv = jnp.zeros((rows, carried.shape[1]), f32)
    for tap in range(3):
        same = (near_doc[tap : tap + rows] == near_doc[1 : rows + 1])[:, None]
        conv = conv + jnp.where(
            same, carry_ext[tap : tap + rows].astype(f32) * taps[tap][None, :], 0.0
        )
    convolved = (bgate * (conv + conv_bias[None, :])).astype(bf16)
    acc = jnp.dot(
        lax.all_gather(attended, "tp", axis=1, tiled=True), w_attn, preferred_element_type=f32
    )
    mixed = acc + jnp.dot(
        lax.all_gather(convolved, "tp", axis=1, tiled=True), w_conv, preferred_element_type=f32
    )
    return mixed.astype(bf16)


def solution(mesh):
    placed = (
        P(("grp", "sp"), "tp"),
        P(),
        P("sp", "tp"),
        P("sp", "tp"),
        P("sp", "tp"),
        P("sp", "tp"),
        P("sp", "tp"),
        P("sp", "tp"),
        P("sp", "tp"),
        P("sp", "tp"),
        P("tp"),
        P(None, "tp"),
        P("tp"),
        P(("grp", "sp")),
    )
    return jax.shard_map(
        local, mesh=mesh, in_specs=placed, out_specs=P(("grp", "sp"), "tp"), check_vma=False
    )
```

```python
import functools

import jax
import jax.numpy as jnp
from jax import lax
from jax.experimental import pallas as pl
from jax.experimental.pallas import tpu as pltpu
from jax.sharding import PartitionSpec as P

HEAD_DIM = 64
WINDOW = 128


EPS = 1e-06
THETA = 500000.0
CONV_UNITS = 4
ATT_UNITS = 2
OUT_UNITS = 2
LATE = 3
TOKEN_CHUNKS = 4


def fused_plan(grp_count, sp_count, tp_count, rows, part, proj_rows, out_rows, q_width, k_width, c_width):
    lines = sp_count // 2
    return (
        grp_count == 2
        and tp_count == 2
        and sp_count % 2 == 0
        and 2 <= lines <= 4
        and proj_rows % (2 * CONV_UNITS * 16) == 0
        and proj_rows % (2 * ATT_UNITS * 16) == 0
        and out_rows % (2 * OUT_UNITS * 16) == 0
        and rows % (TOKEN_CHUNKS * 16) == 0
        and rows % (2 * WINDOW) == 0
        and part % 256 == 0
        and q_width % 256 == 0
        and k_width == 128
        and c_width % 256 == 0
        and 2 * HEAD_DIM == 128
    )


def layer_kernel(
    sizes,
    tok_ref,
    gain_ref,
    wk_ref,
    wv_ref,
    wc_ref,
    wu_ref,
    wb_ref,
    wq_ref,
    wa_ref,
    wm_ref,
    sink_ref,
    taps_ref,
    bias_ref,
    doc_ref,
    doc_col,
    cos_ref,
    sin_ref,
    out_ref,
    wp_full,
    wo_full,
    tok_other,
    scaled,
    inv_ref,
    proj_ref,
    pair_ext,
    query_s,
    carried,
    carry_near,
    doc_row,
    convolved,
    conv_other,
    attended,
    att_other,
    z_send,
    z_recv,
    y_send,
    y_recv,
    dz_send,
    dz_recv,
    dy_send,
    dy_recv,
    do_send,
    do_recv,
    x_send,
    x_recv,
    own_sem,
    halo_send,
    halo_recv,
    conv_sem,
    att_send,
    att_recv,
):
    lines, rp, ro = sizes
    f32 = jnp.float32
    rows, part = tok_ref.shape
    bf16 = jnp.bfloat16
    k_width, c_width, q_width = wk_ref.shape[1], wc_ref.shape[1], wq_ref.shape[1]
    k_at = 3 * c_width
    q_at = k_at + 2 * k_width
    width = q_at + q_width
    y = lax.axis_index("grp")
    sp = lax.axis_index("sp")
    x = lax.axis_index("tp")
    z, c = sp // 2, sp % 2
    groups_of = []
    for full, size, count, cols in (
        (wp_full, rp, CONV_UNITS, (0, k_at)),
        (wp_full, rp, ATT_UNITS, (k_at, width)),
        (wo_full, ro, OUT_UNITS, (0, 2 * part)),
    ):
        groups_of += [(full, size, size // 2 // count, j, cols) for j in range(count)]
    ends = (CONV_UNITS, CONV_UNITS + ATT_UNITS, CONV_UNITS + ATT_UNITS + OUT_UNITS)
    units_of = (range(0, ends[0]), range(ends[0], ends[1]), range(ends[1], ends[2]))
    to_y = {"grp": 1 - y}
    to_core = {"sp": z * 2 + 1 - c}
    to_x = {"tp": 1 - x}
    to_z = ({"sp": sp + 2}, {"sp": sp - 2})
    has_next = (z < lines - 1, z > 0)

    def origin(way, t):
        return z - t if way == 0 else z + t

    def arrives(way, t):
        return z >= t if way == 0 else z < lines - t

    def place(u, zo, cc, h):
        full, size, tall, j, cols = groups_of[u]
        row = (zo * 2 + cc) * size + h * (size // 2) + j * tall
        return full.at[pl.ds(pl.multiple_of(row, tall), tall), cols[0] : cols[1]]

    def remote(src, dst, send, recv, device):
        return pltpu.make_async_remote_copy(
            src_ref=src, dst_ref=dst, send_sem=send, recv_sem=recv,
            device_id=device, device_id_type=pl.DeviceIdType.MESH,
        )

    def z_copy(way, t, u):
        zo = origin(way, t)
        dst = place(u, zo, c, y)
        return remote(dst, dst, z_send.at[way, t, u], z_recv.at[way, t, u], to_z[way])

    def z_arrival(way, t, u):
        dst = place(u, origin(way, t), c, y)
        return remote(dst, dst, z_send.at[way, t - 1, u], z_recv.at[way, t - 1, u], to_z[way])

    def y_copy(way, t, u):
        ref = place(u, origin(way, t), c, y)
        return remote(ref, ref, y_send.at[way, t - 1, u], y_recv.at[way, t - 1, u], to_y)

    def y_arrival(way, t, u):
        ref = place(u, origin(way, t), c, 1 - y)
        return remote(ref, ref, y_send.at[way, t - 1, u], y_recv.at[way, t - 1, u], to_y)

    def d_copy(kind, way, t, u, cc):
        send, recv = (dz_send, dz_recv) if kind == 0 else (dy_send, dy_recv)
        ref = place(u, origin(way, t), cc, y if kind == 0 else 1 - y)
        return remote(ref, ref, send.at[way, t - 1, u], recv.at[way, t - 1, u], to_core)

    def shard(group, cc):
        full, size, _, _, cols = groups_of[ends[group] - 1]
        return full, pl.ds(pl.multiple_of((z * 2 + cc) * size, size), size), cols

    def own_d(group, cc):
        full, at, cols = shard(group, cc)
        dst = full.at[at, cols[0] : cols[1]]
        return remote(dst, dst, do_send.at[group], do_recv.at[group], to_core)

    own_refs = ((wc_ref, wu_ref, wb_ref), (wk_ref, wv_ref, wq_ref), (wa_ref, wm_ref))

    def own_local(group):
        full, at, cols = shard(group, c)
        copies, col = [], cols[0]
        for j, ref in enumerate(own_refs[group]):
            size = ref.shape[1]
            copies.append(
                pltpu.make_async_copy(
                    ref, full.at[at, col : col + size], own_sem.at[3 * group + j]
                )
            )
            col += size
        return copies

    chunk = rows // TOKEN_CHUNKS

    def x_copy(k):
        return remote(
            tok_ref.at[pl.ds(k * chunk, chunk), :], tok_other.at[pl.ds(k * chunk, chunk), :],
            x_send.at[k], x_recv.at[k], to_x,
        )

    last = 2 * lines - 1
    steps_sp = (sp + 1, sp - 1)
    sends_to = (sp < last, sp > 0)
    gets_from = (sp > 0, sp < last)
    side = jnp.where(c == 0, sp - 1, sp + 1)
    has_side = (side >= 0) & (side <= last)

    def halo(kind, way):
        if kind == 0:
            src = doc_ref.at[:, rows - WINDOW : rows] if way == 0 else doc_ref.at[:, 0:WINDOW]
            at = 0 if way == 0 else WINDOW + rows
            dst = doc_row.at[:, at : at + WINDOW]
        elif kind == 1:
            at = rows if way == 0 else WINDOW
            src = pair_ext.at[at : at + WINDOW, :]
            at = 0 if way == 0 else WINDOW + rows
            dst = pair_ext.at[at : at + WINDOW, :]
        else:
            at = rows - 16 if way == 0 else 0
            src = carried.at[at : at + 16, :]
            dst = carry_near.at[way]
        return remote(
            src, dst, halo_send.at[kind, way], halo_recv.at[kind, way], {"sp": steps_sp[way]}
        )

    def start_halo(kind):
        for way in range(2):

            @pl.when(sends_to[way])
            def _():
                halo(kind, way).start()

    def wait_halo(kind):
        for way in range(2):

            @pl.when(gets_from[way])
            def _():
                halo(kind, way).wait_recv()

    def conv_copy():
        return remote(convolved, conv_other, conv_sem.at[0], conv_sem.at[1], to_x)

    def att_copy(i):
        at = pl.ds(pl.multiple_of(i * WINDOW, WINDOW), WINDOW)
        return remote(attended.at[at, :], att_other.at[at, :], att_send.at[i], att_recv.at[i], to_x)

    for copy in own_local(0) + own_local(1) + own_local(2):
        copy.start()

    barrier = pltpu.get_barrier_semaphore()
    for device in (to_y, to_core, to_x):
        pl.semaphore_signal(barrier, inc=1, device_id=device, device_id_type=pl.DeviceIdType.MESH)
    for way in range(2):

        @pl.when(has_next[way])
        def _():
            pl.semaphore_signal(
                barrier, inc=1, device_id=to_z[way], device_id_type=pl.DeviceIdType.MESH
            )

    @pl.when(has_side)
    def _():
        pl.semaphore_signal(
            barrier, inc=1, device_id={"sp": side}, device_id_type=pl.DeviceIdType.MESH
        )

    neighbours = jnp.where(has_side, 1, 0) + jnp.where(z > 0, 1, 0) + jnp.where(z < lines - 1, 1, 0) + 3
    pl.semaphore_wait(barrier, neighbours)

    def start_own(units):
        for u in units:
            for way in range(2):

                @pl.when(has_next[way])
                def _():
                    z_copy(way, 0, u).start()

    for k in range(TOKEN_CHUNKS):
        x_copy(k).start()
    for copy in own_local(0):
        copy.wait()
    start_own(units_of[0])
    own_d(0, c).start()
    start_halo(0)
    doc_row[:, WINDOW : WINDOW + rows] = doc_ref[...]

    @pl.when(sp == 0)
    def _():
        doc_row[:, :WINDOW] = jnp.full((doc_row.shape[0], WINDOW), -1.0, f32)
        pair_ext[:WINDOW, :] = jnp.zeros((WINDOW, pair_ext.shape[1]), bf16)

    @pl.when(sp == last)
    def _():
        doc_row[:, WINDOW + rows :] = jnp.full((doc_row.shape[0], WINDOW), -1.0, f32)
        pair_ext[WINDOW + rows :, :] = jnp.zeros((WINDOW, pair_ext.shape[1]), bf16)


    def event(t, u):
        for way in range(2):

            @pl.when(arrives(way, t))
            def _():
                z_arrival(way, t, u).wait_recv()
                if t < lines - 1:

                    @pl.when(has_next[way])
                    def _():
                        z_copy(way, t, u).start()

                y_copy(way, t, u).start()
                d_copy(0, way, t, u, c).start()

    def y_event(t, u):
        for way in range(2):

            @pl.when(arrives(way, t))
            def _():
                y_arrival(way, t, u).wait_recv()
                d_copy(1, way, t, u, c).start()

    def scale(k):
        x_copy(k).wait_recv()
        tile = 32

        def body(i, carry):
            at = pl.ds(pl.multiple_of(k * chunk + i * tile, tile), tile)
            own = tok_ref[at, :].astype(f32)
            other = tok_other[at, :].astype(f32)
            total = jnp.sum(own * own, axis=1, keepdims=True) + jnp.sum(
                other * other, axis=1, keepdims=True
            )
            inv_ref[at, :] = jnp.broadcast_to(
                lax.rsqrt(total / (2 * part) + EPS), (tile, inv_ref.shape[1])
            )
            mine_at = pl.multiple_of(x * part, part)
            other_at = pl.multiple_of((1 - x) * part, part)
            scaled[at, pl.ds(mine_at, part)] = (own * gain_ref[:, pl.ds(mine_at, part)]).astype(
                scaled.dtype
            )
            scaled[at, pl.ds(other_at, part)] = (
                other * gain_ref[:, pl.ds(other_at, part)]
            ).astype(scaled.dtype)
            return carry

        lax.fori_loop(0, chunk // tile, body, 0)

    queue, marks = [], []
    for units in units_of:
        queue += [(t, u) for t in range(1, lines) for u in units]
        marks.append(len(queue))
    openers = {marks[g] - len(units_of[g]): g + 1 for g in range(2)}
    state = [0, 0]

    def advance(goal):
        while state[0] < goal:
            i = state[0]
            event(*queue[i])
            if i in openers:
                group = openers[i]
                for copy in own_local(group):
                    copy.wait()
                start_own(units_of[group])
                own_d(group, c).start()
            state[0] += 1
            while state[1] < state[0] - LATE:
                y_event(*queue[state[1]])
                state[1] += 1

    def settle(group):
        advance(marks[group])
        while state[1] < marks[group]:
            y_event(*queue[state[1]])
            state[1] += 1
        own_d(group, 1 - c).wait_recv()
        for t, u in queue[marks[group - 1] if group else 0 : marks[group]]:
            for way in range(2):

                @pl.when(arrives(way, t))
                def _():
                    d_copy(0, way, t, u, 1 - c).wait_recv()
                    d_copy(1, way, t, u, 1 - c).wait_recv()

    for k in range(TOKEN_CHUNKS - 1):
        advance(marks[0] * (k + 1) // (TOKEN_CHUNKS - 1))
        scale(k)
    advance(marks[0] + 2)
    settle(0)
    scale(TOKEN_CHUNKS - 1)

    cut = 256
    c_at, u_at, b_at = 0, c_width, 2 * c_width

    def project(begin, end):
        def body(j, carry):
            at = pl.ds(pl.multiple_of(j * cut, cut), cut)
            acc = jnp.dot(scaled[...], wp_full[:, at], preferred_element_type=f32)
            proj_ref[:, at] = acc * inv_ref[:, :1]
            return carry

        lax.fori_loop(begin // cut, end // cut, body, 0)

    lanes = 128
    lane = lax.broadcasted_iota(jnp.int32, (rows, lanes), 1)
    low = (lane % HEAD_DIM) < HEAD_DIM // 2

    def turned(cells):
        ahead = pltpu.roll(cells, lanes - HEAD_DIM // 2, 1)
        behind = pltpu.roll(cells, HEAD_DIM // 2, 1)
        return cells * cos_ref[...] + jnp.where(low, ahead, behind) * sin_ref[...]

    def block(at, j):
        return pl.ds(pl.multiple_of(at + j * lanes, lanes), lanes)

    project(c_at, b_at)

    def carry_body(j, carry):
        carried[:, block(0, j)] = (
            proj_ref[:, block(c_at, j)] * proj_ref[:, block(u_at, j)]
        ).astype(bf16)
        return carry

    lax.fori_loop(0, c_width // lanes, carry_body, 0)
    advance(marks[0] + 3)
    start_halo(2)
    project(b_at, k_at)
    advance(marks[0] + 4)
    wait_halo(0)
    wait_halo(2)

    row = lax.broadcasted_iota(jnp.int32, (rows, lanes), 0)

    def conv_body(j, carry):
        at = block(0, j)
        docs = doc_col[...]
        cells = carried[:, at].astype(f32)
        before = jnp.where(row == 0, carry_near[0, 15:16, at].astype(f32), pltpu.roll(cells, 1, 0))
        after = jnp.where(
            row == rows - 1, carry_near[1, 0:1, at].astype(f32), pltpu.roll(cells, rows - 1, 0)
        )
        doc_before = jnp.where(row == 0, doc_row[0:1, WINDOW - 1 : WINDOW], pltpu.roll(docs, 1, 0))
        doc_after = jnp.where(
            row == rows - 1,
            doc_row[0:1, WINDOW + rows : WINDOW + rows + 1],
            pltpu.roll(docs, rows - 1, 0),
        )
        conv = jnp.where(doc_before == docs, before * taps_ref[0:1, at], 0.0)
        conv = conv + cells * taps_ref[1:2, at]
        conv = conv + jnp.where(doc_after == docs, after * taps_ref[2:3, at], 0.0)
        convolved[:, at] = (proj_ref[:, block(b_at, j)] * (conv + bias_ref[:, at])).astype(bf16)
        return carry

    lax.fori_loop(0, c_width // lanes, conv_body, 0)
    conv_copy().start()
    settle(1)
    project(k_at, q_at)
    keys_at = slice(k_at, k_at + k_width)
    pair_ext[WINDOW : WINDOW + rows, :k_width] = turned(proj_ref[:, keys_at]).astype(bf16)
    pair_ext[WINDOW : WINDOW + rows, k_width:] = proj_ref[:, k_at + k_width : q_at].astype(bf16)
    start_halo(1)
    advance(marks[1] + 1)
    project(q_at, width)
    advance(marks[1] + 2)

    def query_body(j, carry):
        cells = turned(proj_ref[:, block(q_at, j)])
        query_s[:, block(0, j)] = (cells * HEAD_DIM ** (-0.5)).astype(bf16)
        return carry

    lax.fori_loop(0, q_width // lanes, query_body, 0)
    wait_halo(1)
    kv_heads = k_width // HEAD_DIM
    groups = q_width // HEAD_DIM // kv_heads
    span = 3 * WINDOW
    gap = lax.broadcasted_iota(jnp.int32, (WINDOW, span), 1) - lax.broadcasted_iota(
        jnp.int32, (WINDOW, span), 0
    )
    window = (gap >= 0) & (gap <= 2 * WINDOW)

    def attend(i, carry):
        at = pl.ds(pl.multiple_of(i * WINDOW, WINDOW), WINDOW)
        near = pl.ds(pl.multiple_of(i * WINDOW, WINDOW), span)
        allowed = window & (doc_col[at, 0:1] == doc_row[0:1, near])
        bias = jnp.where(allowed, 0.0, -jnp.inf)
        bias = jnp.concatenate([bias] * groups, axis=0)
        queries = query_s[at, :]
        pairs = pair_ext[near, :]
        for head in range(kv_heads):
            keys = pairs[:, head * HEAD_DIM : (head + 1) * HEAD_DIM]
            values = pairs[:, k_width + head * HEAD_DIM : k_width + (head + 1) * HEAD_DIM]
            first = head * groups
            stack = jnp.concatenate(
                [
                    queries[:, (first + g) * HEAD_DIM : (first + g + 1) * HEAD_DIM]
                    for g in range(groups)
                ],
                axis=0,
            )
            sinks = jnp.concatenate(
                [jnp.full((WINDOW, 1), sink_ref[first + g], f32) for g in range(groups)], axis=0
            )
            scores = lax.dot_general(
                stack, keys, (((1,), (1,)), ((), ())), preferred_element_type=f32
            )
            scores = scores + bias
            top = jnp.maximum(jnp.max(scores, axis=1, keepdims=True), sinks)
            expo = jnp.exp(scores - top)
            total = jnp.sum(expo, axis=1, keepdims=True) + jnp.exp(sinks - top)
            weight = (expo * (1.0 / total)).astype(bf16)
            result = jnp.dot(weight, values, preferred_element_type=f32).astype(bf16)
            wide = jnp.concatenate(
                [result[g * WINDOW : (g + 1) * WINDOW] for g in range(groups)], axis=1
            )
            attended[at, first * HEAD_DIM : (first + groups) * HEAD_DIM] = wide

        @pl.when(i > 0)
        def _():
            att_copy(i - 1).start()

        return carry

    blocks = rows // WINDOW
    lax.fori_loop(0, blocks // 2, attend, 0)
    advance(marks[1] + 4)
    lax.fori_loop(blocks // 2, blocks, attend, 0)
    att_copy(blocks - 1).start()
    settle(2)
    conv_copy().wait_recv()
    q_mine = pl.ds(pl.multiple_of(x * q_width, q_width), q_width)
    q_yours = pl.ds(pl.multiple_of((1 - x) * q_width, q_width), q_width)
    c_mine = pl.ds(pl.multiple_of(x * c_width, c_width), c_width)
    c_yours = pl.ds(pl.multiple_of((1 - x) * c_width, c_width), c_width)

    def mix_body(j, carry):
        at = pl.ds(pl.multiple_of(j * cut, cut), cut)
        late = pl.ds(pl.multiple_of(part + j * cut, cut), cut)
        acc = jnp.dot(attended[...], wo_full[q_mine, at], preferred_element_type=f32)
        acc = acc + jnp.dot(convolved[...], wo_full[c_mine, late], preferred_element_type=f32)
        acc = acc + jnp.dot(conv_other[...], wo_full[c_yours, late], preferred_element_type=f32)
        proj_ref[:, at] = acc
        return carry

    lax.fori_loop(0, part // cut, mix_body, 0)
    half = rows // 2
    for k in range(2):
        for i in range(k * blocks // 2, (k + 1) * blocks // 2):
            att_copy(i).wait_recv()

        def last_body(j, carry):
            at = pl.ds(pl.multiple_of(j * cut, cut), cut)
            acc = proj_ref[k * half : (k + 1) * half, at] + jnp.dot(
                att_other[k * half : (k + 1) * half, :],
                wo_full[q_yours, at],
                preferred_element_type=f32,
            )
            out_ref[k * half : (k + 1) * half, at] = acc.astype(bf16)
            return carry

        lax.fori_loop(0, part // cut, last_body, 0)

    for kind in range(3):
        for way in range(2):

            @pl.when(sends_to[way])
            def _():
                halo(kind, way).wait_send()

    conv_copy().wait_send()
    for i in range(blocks):
        att_copy(i).wait_send()
    for group in range(3):
        own_d(group, c).wait_send()
    for k in range(TOKEN_CHUNKS):
        x_copy(k).wait_send()
    for u in range(ends[2]):
        for way in range(2):

            @pl.when(has_next[way])
            def _():
                z_copy(way, 0, u).wait_send()

            for t in range(1, lines):

                @pl.when(arrives(way, t))
                def _():
                    if t < lines - 1:

                        @pl.when(has_next[way])
                        def _():
                            z_copy(way, t, u).wait_send()

                    y_copy(way, t, u).wait_send()
                    d_copy(0, way, t, u, c).wait_send()
                    d_copy(1, way, t, u, c).wait_send()


def fused_layer(
    tokens, gain, projections, outputs, sink_logit, taps, conv_bias, documents, sp_count
):
    rows, part = tokens.shape
    f32 = jnp.float32
    bf16 = jnp.bfloat16
    lines = sp_count // 2
    wk, wv, wc, wu, wb, wq = projections
    width = sum(w.shape[1] for w in projections)
    rp, ro = wq.shape[0], outputs[0].shape[0]
    q_width, k_width, c_width = wq.shape[1], wk.shape[1], wc.shape[1]
    half = HEAD_DIM // 2
    lanes = 128
    positions = lax.axis_index("sp") * rows + jnp.arange(rows, dtype=jnp.int32)
    freq = jnp.power(THETA, -(jnp.arange(half, dtype=f32) * (2.0 / HEAD_DIM)))
    angle = positions.astype(f32)[:, None] * freq[None, :]
    cosine, sine = jnp.cos(angle), jnp.sin(angle)
    cosine = jnp.concatenate([cosine] * (lanes // half), axis=1)
    sine = jnp.concatenate([-sine, sine] * (lanes // HEAD_DIM), axis=1)
    docs = documents.astype(f32)
    doc_rows = jnp.broadcast_to(docs[None, :], (8, rows))
    doc_cols = jnp.broadcast_to(docs[:, None], (rows, lanes))
    blocks = rows // WINDOW
    dma = pltpu.SemaphoreType.DMA
    hops = (2, lines - 1, CONV_UNITS + ATT_UNITS + OUT_UNITS)
    vmem = pl.BlockSpec(memory_space=pltpu.VMEM)
    hbm = pl.BlockSpec(memory_space=pl.ANY)
    smem = pl.BlockSpec(memory_space=pltpu.SMEM)
    flops = 2 * rows * 2 * part * width
    return pl.pallas_call(
        functools.partial(layer_kernel, (lines, rp, ro)),
        out_shape=jax.ShapeDtypeStruct((rows, part), bf16),
        in_specs=[vmem] * 2 + [hbm] * 8 + [smem] + [vmem] * 6,
        out_specs=vmem,
        scratch_shapes=[
            pltpu.VMEM((rp * sp_count, width), bf16),
            pltpu.VMEM((ro * sp_count, 2 * part), bf16),
            pltpu.VMEM((rows, part), bf16),
            pltpu.VMEM((rows, 2 * part), bf16),
            pltpu.VMEM((rows, 128), f32),
            pltpu.VMEM((rows, max(width, part)), f32),
            pltpu.VMEM((rows + 2 * WINDOW, 2 * k_width), bf16),
            pltpu.VMEM((rows, q_width), bf16),
            pltpu.VMEM((rows, c_width), bf16),
            pltpu.VMEM((2, 16, c_width), bf16),
            pltpu.VMEM((8, rows + 2 * WINDOW), f32),
            pltpu.VMEM((rows, c_width), bf16),
            pltpu.VMEM((rows, c_width), bf16),
            pltpu.VMEM((rows, q_width), bf16),
            pltpu.VMEM((rows, q_width), bf16),
        ]
        + [dma(hops)] * 8
        + [dma((3,)), dma((3,)), dma((TOKEN_CHUNKS,)), dma((TOKEN_CHUNKS,)), dma((9,))]
        + [dma((3, 2)), dma((3, 2)), dma((2,)), dma((blocks,)), dma((blocks,))],
        compiler_params=pltpu.CompilerParams(
            collective_id=0, has_side_effects=True, vmem_limit_bytes=62 * 1024 * 1024
        ),
        cost_estimate=pl.CostEstimate(flops=flops, bytes_accessed=0, transcendentals=0),
        name="layer",
    )(
        tokens,
        gain[None, :],
        *projections,
        *outputs,
        sink_logit,
        taps,
        conv_bias[None, :],
        doc_rows,
        doc_cols,
        cosine,
        sine,
    )


def extended(cells, sides, width):
    for axis, dim in sides:
        count = lax.axis_size(axis)
        ends = count - 1
        head = lax.slice_in_dim(cells, 0, width, axis=dim)
        tail = lax.slice_in_dim(cells, cells.shape[dim] - width, cells.shape[dim], axis=dim)
        cells = jnp.concatenate(
            [
                lax.ppermute(tail, axis, [(i, (i + 1) % count) for i in range(ends)]),
                cells,
                lax.ppermute(head, axis, [((i + 1) % count, i) for i in range(ends)]),
            ],
            axis=dim,
        )
    return cells


def rotate(proj, positions, heads):
    rows = proj.shape[0]
    size = proj.shape[1] // heads
    half = size // 2
    freq = jnp.power(THETA, -(jnp.arange(half, dtype=jnp.float32) * (2.0 / size)))
    angle = positions.astype(jnp.float32)[:, None] * freq[None, :]
    cosine = jnp.cos(angle)[:, None, :]
    sine = jnp.sin(angle)[:, None, :]
    shaped = proj.reshape(rows, heads, size)
    first = shaped[..., :half]
    second = shaped[..., half:]
    turned = jnp.concatenate(
        [first * cosine - second * sine, second * cosine + first * sine], axis=-1
    )
    return turned.reshape(rows, heads * size)


def sink_softmax(scores, allowed, sinks):
    masked = jnp.where(allowed, scores, -jnp.inf)
    top = jnp.maximum(jnp.max(masked, axis=-1, keepdims=True), sinks)
    expo = jnp.exp(masked - top)
    return expo / (jnp.sum(expo, axis=-1, keepdims=True) + jnp.exp(sinks - top))


def local(
    tokens,
    gain,
    w_query,
    w_key,
    w_value,
    w_input,
    w_bgate,
    w_cgate,
    w_attn_out,
    w_conv_out,
    sink_logit,
    taps,
    conv_bias,
    documents,
):
    f32 = jnp.float32
    bf16 = jnp.bfloat16
    rows, part = tokens.shape
    tp_count = lax.axis_size("tp")
    sp_count = lax.axis_size("sp")
    width = part * tp_count
    head_dim = HEAD_DIM
    q_local = w_query.shape[1] // head_dim
    kv_local = w_key.shape[1] // head_dim
    groups = q_local // kv_local
    if fused_plan(
        lax.axis_size("grp"),
        sp_count,
        tp_count,
        rows,
        part,
        w_query.shape[0],
        w_attn_out.shape[0],
        w_query.shape[1],
        w_key.shape[1],
        w_input.shape[1],
    ):
        return fused_layer(
            tokens,
            gain,
            (w_key, w_value, w_cgate, w_input, w_bgate, w_query),
            (w_attn_out, w_conv_out),
            sink_logit,
            taps,
            conv_bias,
            documents,
            sp_count,
        )
    wq, wk, wv, wu, wb, wc, w_attn, w_conv = (
        lax.all_gather(w_query, "sp", axis=0, tiled=True),
        lax.all_gather(w_key, "sp", axis=0, tiled=True),
        lax.all_gather(w_value, "sp", axis=0, tiled=True),
        lax.all_gather(w_input, "sp", axis=0, tiled=True),
        lax.all_gather(w_bgate, "sp", axis=0, tiled=True),
        lax.all_gather(w_cgate, "sp", axis=0, tiled=True),
        lax.all_gather(w_attn_out, "sp", axis=0, tiled=True),
        lax.all_gather(w_conv_out, "sp", axis=0, tiled=True),
    )
    matrices = (wq, wk, wv, wu, wb, wc)
    piece_f = lax.all_gather(tokens, "tp", axis=1, tiled=True).astype(f32)
    scaled = (piece_f * gain[None, :]).astype(bf16)
    products = tuple((jnp.dot(scaled, mat, preferred_element_type=f32) for mat in matrices))
    folded = products + (jnp.sum(piece_f * piece_f, axis=1),)
    sums = folded[:6]
    squares = folded[6]
    inv = lax.rsqrt(squares / width + EPS)[:, None]
    q_acc, k_acc, v_acc, u_acc, b_acc, c_acc = sums
    positions = lax.axis_index("sp") * rows + jnp.arange(rows, dtype=jnp.int32)
    query = rotate(q_acc * inv, positions, q_local).astype(bf16)
    keys = rotate(k_acc * inv, positions, kv_local).astype(bf16)
    values = (v_acc * inv).astype(bf16)
    carried = (c_acc * inv * (u_acc * inv)).astype(bf16)
    bgate = b_acc * inv
    doc_col = documents.astype(f32).astype(bf16)[:, None]
    paired = jnp.concatenate([keys, values], axis=1)
    pair_ext, doc_ext = (
        extended(paired, (("sp", 0),), WINDOW),
        extended(doc_col, (("sp", 0),), WINDOW),
    )
    carry_ext, doc_near = (extended(carried, (("sp", 0),), 1), extended(doc_col, (("sp", 0),), 1))
    key_width = kv_local * head_dim
    key_ext = pair_ext[:, :key_width].reshape(-1, kv_local, head_dim)
    val_ext = pair_ext[:, key_width:].reshape(-1, kv_local, head_dim)
    key_doc = doc_ext[:, 0].astype(f32)
    own_doc = doc_col[:, 0].astype(f32)
    key_pos = positions[0] - WINDOW + jnp.arange(rows + 2 * WINDOW, dtype=jnp.int32)
    total = sp_count * rows
    sinks = sink_logit.reshape(kv_local, groups, 1, 1)
    block = rows // 2
    outputs = []
    for begin in range(0, rows, block):
        span = block + 2 * WINDOW
        q_block = query[begin : begin + block].reshape(block, kv_local, groups, head_dim)
        k_block = key_ext[begin : begin + span]
        v_block = val_ext[begin : begin + span]
        q_pos = positions[begin : begin + block]
        k_pos = key_pos[begin : begin + span]
        scores = jnp.einsum(
            "qhgd,khd->hgqk", q_block, k_block, preferred_element_type=f32
        ) * head_dim ** (-0.5)
        allowed = jnp.abs(q_pos[:, None] - k_pos[None, :]) <= WINDOW
        allowed = allowed & (
            own_doc[begin : begin + block, None] == key_doc[None, begin : begin + span]
        )
        allowed = allowed & (k_pos >= 0)[None, :] & (k_pos < total)[None, :]
        weight = sink_softmax(scores, allowed, sinks).astype(bf16)
        result = jnp.einsum("hgqk,khd->qhgd", weight, v_block, preferred_element_type=f32)
        outputs.append(result.astype(bf16).reshape(block, q_local * head_dim))
    attended = jnp.concatenate(outputs, axis=0)
    near_doc = doc_near[:, 0].astype(f32)
    conv = jnp.zeros((rows, carried.shape[1]), f32)
    for tap in range(3):
        same = (near_doc[tap : tap + rows] == near_doc[1 : rows + 1])[:, None]
        conv = conv + jnp.where(
            same, carry_ext[tap : tap + rows].astype(f32) * taps[tap][None, :], 0.0
        )
    convolved = (bgate * (conv + conv_bias[None, :])).astype(bf16)
    acc = jnp.dot(
        lax.all_gather(attended, "tp", axis=1, tiled=True), w_attn, preferred_element_type=f32
    )
    mixed = acc + jnp.dot(
        lax.all_gather(convolved, "tp", axis=1, tiled=True), w_conv, preferred_element_type=f32
    )
    return mixed.astype(bf16)


def solution(mesh):
    placed = (
        P(("grp", "sp"), "tp"),
        P(),
        P("sp", "tp"),
        P("sp", "tp"),
        P("sp", "tp"),
        P("sp", "tp"),
        P("sp", "tp"),
        P("sp", "tp"),
        P("sp", "tp"),
        P("sp", "tp"),
        P("tp"),
        P(None, "tp"),
        P("tp"),
        P(("grp", "sp")),
    )
    return jax.shard_map(
        local, mesh=mesh, in_specs=placed, out_specs=P(("grp", "sp"), "tp"), check_vma=False
    )
```
